512 devices in a mesh: ep: 32 (over z, core), tp: 16 (over y, x).
Axes of the slice: x: 4, y: 4, z: 16, core: 2. Of those that a mesh axis runs over, the one named last changes fastest.
Arguments:
- tokens: bfloat16 [65536, 2048], P(('ep', 'tp')), may hold values from -6 to 6
- norm_gain: float32 [2048], replicated, may hold values from 0.1 to 1.9
- expert_ids: int32 [65536, 2], P(('ep', 'tp')), may hold values from 0 to 31, all different within a row; in each aligned block of 128 rows (0 to 127, 128 to 255, ...) at most 16 rows name the same one
- gate_weights: float32 [65536, 2], P(('ep', 'tp')), may hold values from 0.2 to 1.6
- expert_gate: bfloat16 [32, 512, 2048], P('ep', 'tp'), may hold values from -0.125 to 0.125
- expert_up: bfloat16 [32, 512, 2048], P('ep', 'tp'), may hold values from -0.125 to 0.125
- expert_down: bfloat16 [32, 512, 2048], P('ep', 'tp'), may hold values from -0.25 to 0.25
- shared_gate: bfloat16 [512, 2048], P('tp'), may hold values from -0.125 to 0.125
- shared_up: bfloat16 [512, 2048], P('tp'), may hold values from -0.125 to 0.125
- shared_down: bfloat16 [512, 2048], P('tp'), may hold values from -0.25 to 0.25
Outputs:
- mixed: bfloat16 [65536, 2048], P(('ep', 'tp'))
The draws below stay inside these ranges and needn't reach their ends.
Inputs may be any that keep to these rules, and one draw needn't show every extreme that they name: `expert_ids`: each row names 2 different experts. Within the rows of one device no expert is named by more than 16 rows, and in every draw some expert is named by exactly 16 rows of some device.
All inputs are finite; a program needn't handle non-finite values.
Results may differ from the reference program's by a relative error of at most 0.0068.
Values may be sent and summed in bfloat16 or wider, within the bound.
A program may use at most 64 MiB of HBM per device.

```python
import math
import jax
import jax.numpy as jnp
import numpy as np
from jax import lax

D = 2048
FF = 512
SFF = 512
K = 2
TOK_DEV = 128
EXPERTS = 32
CAP = 16
TOKENS = 65536


def block_levels(rng, shape, shards, smallest, largest):
    gain = 1.0
    for dim, parts in shards:
        draws = jax.random.uniform(jax.random.fold_in(jax.random.fold_in(rng, 6), dim), (parts,), jnp.float32, smallest / len(shards), largest / len(shards))
        gain = gain * jnp.repeat(jnp.exp(draws), shape[dim] // parts).reshape((-1,) + (1,) * (len(shape) - 1 - dim))
    return gain


def deal_out(own_key, own, number, rows, amount, top, limit, skew):
    sequence = jax.random.permutation(own_key, amount)
    packed, common = shares(amount, rows * top, limit, skew, True), shares(amount, rows * top, limit, skew, False)
    places = jnp.arange(amount)

    def named(tallies, turn):
        used = int((tallies > 0).sum())
        fixed = max(1, used // 4)
        shifted = fixed + (places - fixed + turn * (used - fixed)) % max(1, amount - fixed)
        return jnp.zeros((amount,), jnp.int32).at[sequence[jnp.where(places < fixed, places, shifted)]].set(jnp.asarray(tallies, jnp.int32))

    tallies = jnp.where(number % 4 == 0, named(packed, number // 4), named(common, number - number // 4 - 1))
    mixed = jax.random.permutation(jax.random.fold_in(own, 3), amount)
    giver, taker = mixed[0:amount // 2 * 2:2], mixed[1:amount // 2 * 2:2]
    slack = jnp.minimum(tallies[giver] - 1, limit - tallies[taker]) // 2
    slack = jnp.where((giver == sequence[0]) | (taker == sequence[0]) | (tallies[taker] == 0), 0, jnp.maximum(slack, 0))
    shifted = jax.random.randint(jax.random.fold_in(own, 4), (amount // 2,), 0, 1 << 20) % (slack + 1)
    tallies = tallies.at[giver].add(-shifted).at[taker].add(shifted)
    members = jnp.searchsorted(jnp.cumsum(tallies), jnp.arange(rows * top), side="right").astype(jnp.int32)
    listing = members.reshape(top, rows).T
    listing = listing[jax.random.permutation(jax.random.fold_in(own, 1), rows)]
    turn = jax.random.randint(jax.random.fold_in(own, 2), (rows, 1), 0, top)
    return jnp.take_along_axis(listing, (jnp.arange(top)[None, :] + turn) % top, axis=1)


def shares(amount, total, bound, lean, full):
    portions = [(1 << 20) // math.isqrt(standing ** lean) + 1 for standing in range(1, amount + 1)]
    largest = bound if full else min(bound, max(-(-total // amount), total * portions[0] // sum(portions)))
    least = 1 if total - largest >= amount - 1 else 0
    counts, rest = [largest] + [least] * (amount - 1), total - largest - least * (amount - 1)
    while rest > 0:
        free = [i for i in range(1, amount) if counts[i] < largest] or [i for i in range(1, amount) if counts[i] < bound]
        mass, left = sum([portions[i] for i in free]), rest
        for i in free:
            addition = min(bound - counts[i], max(1, left * portions[i] // mass), rest)
            counts[i] = counts[i] + addition
            rest = rest - addition
    return np.array(counts)


def normal_values(rng, extent, spread, reach, pieces=(), held_as=jnp.bfloat16):
    values = spread * jax.random.normal(rng, extent, jnp.float32)
    if pieces:
        values = values * block_levels(rng, extent, pieces, -0.22, 0.18)
    return jnp.clip(values, -reach, reach).astype(held_as)


def setup_inputs(seed: int = 0) -> dict:
    seeds = jax.random.split(jax.random.key(seed), 11)
    tokens = normal_values(seeds[0], (TOKENS, D), 1.0, 6.0, ((0, 512),))
    norm_gain = jnp.clip(1.0 + 0.18 * jax.random.normal(seeds[1], (D,), jnp.float32), 0.1, 1.9)
    expert_ids_keys = jax.random.split(jax.random.fold_in(seeds[2], 1), TOKENS // TOK_DEV)
    expert_ids_turns = jax.random.permutation(jax.random.fold_in(seeds[2], 3), TOKENS // TOK_DEV)
    expert_ids = jax.vmap(lambda own, number: deal_out(jax.random.fold_in(seeds[2], 2), own, number, TOK_DEV, EXPERTS, K, CAP, 2))(expert_ids_keys, expert_ids_turns).reshape((TOKENS, K))
    gate_weights = jnp.clip(0.2 + 1.4 * jax.random.uniform(seeds[3], (TOKENS, K), jnp.float32) ** block_levels(seeds[3], (TOKENS, K), ((0, 512),), -0.2, 0.2), 0.2, 1.6)
    expert_gate = normal_values(seeds[4], (EXPERTS, FF, D), D ** -0.5, 0.125, ((0, 32), (1, 16)))
    expert_up = normal_values(seeds[5], (EXPERTS, FF, D), D ** -0.5, 0.125, ((0, 32), (1, 16)))
    expert_down = normal_values(seeds[6], (EXPERTS, FF, D), FF ** -0.5, 0.25, ((0, 32), (1, 16)))
    shared_gate = normal_values(seeds[7], (SFF, D), D ** -0.5, 0.125, ((0, 16),))
    shared_up = normal_values(seeds[8], (SFF, D), D ** -0.5, 0.125, ((0, 16),))
    shared_down = normal_values(seeds[9], (SFF, D), SFF ** -0.5, 0.25, ((0, 16),))
    return {"tokens": tokens, "norm_gain": norm_gain, "expert_ids": expert_ids, "gate_weights": gate_weights, "expert_gate": expert_gate, "expert_up": expert_up, "expert_down": expert_down, "shared_gate": shared_gate, "shared_up": shared_up, "shared_down": shared_down}


EPS = 1e-06

def against(rows, weight):
    return jnp.dot(rows, weight.T, preferred_element_type=jnp.float32)

def reference(tokens, norm_gain, expert_ids, gate_weights, expert_gate, expert_up, expert_down, shared_gate, shared_up, shared_down):
    tok = tokens.astype(jnp.float32)
    normed = (tok * lax.rsqrt(lax.optimization_barrier(jnp.mean(tok * tok, axis=-1, keepdims=True)) + EPS) * norm_gain).astype(jnp.bfloat16)
    most_rows = TOKENS // TOK_DEV * CAP
    order = jnp.arange(TOKENS, dtype=jnp.int32)

    def one_expert(index, routed):
        named = expert_ids == index
        member = jnp.any(named, axis=1).astype(jnp.int32)
        weight_row = lax.optimization_barrier(jnp.sum(jnp.where(named, gate_weights, 0.0), axis=1))
        place = (jnp.cumsum(member) - member).astype(jnp.int32)
        place = jnp.where(member > 0, place, most_rows).astype(jnp.int32)
        table = jnp.full((most_rows,), TOKENS, jnp.int32).at[place].set(order, mode='drop')
        rows = jnp.take(normed, table, axis=0, mode='fill', fill_value=0)
        scale = jnp.take(weight_row, table, axis=0, mode='fill', fill_value=0)
        gate = lax.dynamic_index_in_dim(expert_gate, index, 0, keepdims=False)
        up = lax.dynamic_index_in_dim(expert_up, index, 0, keepdims=False)
        down = lax.dynamic_index_in_dim(expert_down, index, 0, keepdims=False)
        hidden = (jax.nn.silu(against(rows, gate)) * against(rows, up)).astype(jnp.bfloat16)
        result = jnp.dot(hidden, down, preferred_element_type=jnp.float32).astype(jnp.bfloat16)
        return routed.at[table].add(scale[:, None] * result.astype(jnp.float32), mode='drop')
    routed = lax.fori_loop(0, EXPERTS, one_expert, jnp.zeros((TOKENS, D), jnp.float32))
    shared_hidden = (jax.nn.silu(against(normed, shared_gate)) * against(normed, shared_up)).astype(jnp.bfloat16)
    shared = jnp.dot(shared_hidden, shared_down, preferred_element_type=jnp.float32)
    return (routed + shared).astype(jnp.bfloat16)
```

```python
import functools

import jax
import jax.numpy as jnp
from jax import lax
from jax.experimental import pallas as pl
from jax.experimental.pallas import tpu as pltpu
from jax.sharding import PartitionSpec as P

EPS = 1e-06
MESH = pl.DeviceIdType.MESH
BF = jnp.bfloat16
F32 = jnp.float32
NX = 4
NZ = 16
TOK = 128
D = 2048
CAP = 16
NE = 32
COLS = 512
ND = D // COLS
NT = (((1,), (1,)), ((), ()))


def kernel(
    tokens, gain, ids, gw, eg, eu, ed, shg, shu, shd, out,
    tok, xt, meta, sw, part, pin, own, placed, rows, hid, wgu, wd, res, ret, wt, outb,
    zrecv, zsend, gsend, loc, xrecv, mrecv, srecv, prow, pinr, retr, sends, osem,
):
    ep, p = lax.axis_index("ep"), lax.axis_index("tp")
    z, c = ep // 2, ep % 2
    x, y = p % NX, p // NX
    delta = (z - (p + 8 * c) + 2 * NZ) % NZ
    go_up = delta <= 7
    go_down = (delta == 0) | (delta >= 10)
    ep_up = ((z + 1) % NZ) * 2 + c
    ep_down = ((z + NZ - 1) % NZ) * 2 + c
    target = (z + 8 * c) % NZ
    here = p == target

    def arrived(ref, sem):
        pltpu.make_async_copy(ref, ref, sem).wait()

    def send(src, dst, ssem, rsem, device):
        pltpu.make_async_remote_copy(
            src_ref=src, dst_ref=dst, send_sem=ssem, recv_sem=rsem,
            device_id=device, device_id_type=MESH,
        ).start()

    pltpu.make_async_copy(tokens, tok, loc).start()
    for m, ref in enumerate((shg, shu, shd)):
        pltpu.make_async_copy(ref, sw.at[m, y], srecv.at[y]).start()

    barrier = pltpu.get_barrier_semaphore()

    def greet(i, carry):
        @pl.when(jnp.logical_or(i // 2 != p, i % 2 != c))
        def _():
            pl.semaphore_signal(barrier, inc=1, device_id=(z * 2 + i % 2, i // 2), device_id_type=MESH)
        return carry

    lax.fori_loop(0, NE, greet, 0)
    pl.semaphore_signal(barrier, inc=1, device_id=(ep_up, p), device_id_type=MESH)
    pl.semaphore_signal(barrier, inc=1, device_id=(ep_down, p), device_id_type=MESH)
    pl.semaphore_wait(barrier, NE + 1)

    pieces = []
    for r in range(2):
        pieces.append((eg.at[r], wgu.at[0, r, p], r * 32 + p * 2))
        pieces.append((eu.at[r], wgu.at[1, r, p], r * 32 + p * 2 + 1))
    for n in range(ND):
        cols = pl.ds(n * COLS, COLS)
        pieces.append((ed.at[:, :, cols], wd.at[:, p, :, cols], 64 + n * 16 + p))

    @pl.when(here)
    def _():
        for src, dst, k in pieces:
            pltpu.make_async_copy(src, dst, zrecv.at[k]).start()

    @pl.when(jnp.logical_not(here))
    def _():
        for src, dst, k in pieces:
            send(src, dst, gsend, zrecv.at[k], (ep, target))

    ids0, ids1 = ids[0:1, :], ids[1:2, :]
    e_iota = lax.broadcasted_iota(jnp.int32, (NE, TOK), 0)
    h0 = e_iota == ids0
    h1 = e_iota == ids1
    one, zero = jnp.float32(1), jnp.float32(0)
    hits = (jnp.where(h0, one, zero) + jnp.where(h1, one, zero)).astype(BF)
    earlier = jnp.where(
        lax.broadcasted_iota(jnp.int32, (TOK, TOK), 0) < lax.broadcasted_iota(jnp.int32, (TOK, TOK), 1), one, zero
    ).astype(BF)
    before = jnp.dot(hits, earlier, preferred_element_type=F32)
    slot0 = jnp.sum(jnp.where(h0, before, zero), axis=0, keepdims=True)
    slot1 = jnp.sum(jnp.where(h1, before, zero), axis=0, keepdims=True)
    pos0 = ids0.astype(F32) * CAP + slot0
    pos1 = ids1.astype(F32) * CAP + slot1
    sub = lax.broadcasted_iota(jnp.int32, (8, TOK), 0)
    meta[x] = jnp.where(sub == 0, jnp.broadcast_to(pos0, (8, TOK)), jnp.broadcast_to(pos1, (8, TOK)))

    pltpu.make_async_copy(tokens, tok, loc).wait()
    g = gain[...]

    def norm(i, carry):
        at = pl.ds(pl.multiple_of(i * 16, 16), 16)
        t = tok[at, :].astype(F32)
        scale = lax.rsqrt(jnp.mean(t * t, axis=-1, keepdims=True) + EPS)
        xt[x, at, :] = (t * scale * g).astype(BF)
        return carry

    lax.fori_loop(0, TOK // 16, norm, 0)
    for i in (1, 3, 2):
        peer = (ep, y * NX + (x + i) % NX)
        send(meta.at[x], meta.at[x], sends.at[0], mrecv.at[x], peer)
        send(xt.at[x], xt.at[x], sends.at[1], xrecv.at[x], peer)
    for i in (1, 3, 2):
        peer = (ep, ((y + i) % NX) * NX + x)
        for m, ref in enumerate((shg, shu, shd)):
            send(ref, sw.at[m, y], sends.at[2], srecv.at[y], peer)

    slot_iota = lax.broadcasted_iota(jnp.int32, (NE * CAP, TOK), 0).astype(F32)
    w = jnp.where(slot_iota == pos0, gw[0:1, :], zero) + jnp.where(slot_iota == pos1, gw[1:2, :], zero)
    w = w.T
    w_hi = w.astype(BF)
    wt[0] = w_hi
    wt[1] = (w - w_hi.astype(F32)).astype(BF)

    def place(i):
        s = (x + i) % NX
        if i:
            arrived(meta.at[s], mrecv.at[s])
            arrived(xt.at[s], xrecv.at[s])
        row = lax.broadcasted_iota(jnp.int32, (TOK, TOK), 0)
        dest, slot = row >> 4, row & 15
        dy, dc = dest >> 1, dest & 1
        expert = 2 * ((4 * dy + x + 8 * dc) & 15) + dc
        aim = (expert * CAP + slot).astype(F32)
        m = meta[s]
        onehot = jnp.where((aim == m[0:1, :]) | (aim == m[1:2, :]), one, zero).astype(BF)
        for j in range(ND):
            cols = pl.ds(j * COLS, COLS)
            placed[s, :, :, cols] = (
                jnp.dot(onehot, xt[s, :, cols], preferred_element_type=F32).astype(BF).reshape(8, CAP, COLS)
            )
        src = (y * 2 + c) * NX + s
        rows[src] = placed[s, y * 2 + c]
        for q in range(1, 8):
            dest = (y * 2 + c + q) % 8
            send(placed.at[s, dest], rows.at[src], sends.at[3], prow, (z * 2 + dest % 2, (dest // 2) * NX + x))

    def shared(i):
        s = (x + i) % NX
        if i == 0:
            for q in range(NX):
                arrived(sw.at[:, q], srecv.at[q])
        blk = xt[s]
        a = lax.dot_general(blk, sw[0].reshape(TOK, D), NT, preferred_element_type=F32)
        b = lax.dot_general(blk, sw[1].reshape(TOK, D), NT, preferred_element_type=F32)
        h = (a / (1.0 + jnp.exp(-a)) * b).astype(BF)
        down = sw.at[2]
        for j in range(ND):
            cols = pl.ds(j * COLS, COLS)
            v = jnp.dot(h, down[:, :, cols].reshape(TOK, COLS), preferred_element_type=F32)
            if i == 0:
                own[:, cols] = v
            else:
                part[s, :, cols] = v.astype(BF)
        if i:
            send(part.at[s], pin.at[x], sends.at[4], pinr.at[x], (ep, y * NX + s))

    def hidden(r, b):
        if r == 0 and b == 0:
            arrived(rows.at[pl.ds(0, 28)], prow)
        blk = rows[8 * b:8 * b + 8].reshape(TOK, D)
        a = lax.dot_general(blk, wgu[0, r].reshape(256, D), NT, preferred_element_type=F32)
        u = lax.dot_general(blk, wgu[1, r].reshape(256, D), NT, preferred_element_type=F32)
        hid[r, b * TOK:(b + 1) * TOK, :] = (a / (1.0 + jnp.exp(-a)) * u).astype(BF)

    def pass_on(ref, k, which):
        arrived(ref, zrecv.at[k])

        @pl.when(go_up)
        def _():
            send(ref, ref, zsend.at[which], zrecv.at[k], (ep_up, p))

        @pl.when(go_down)
        def _():
            send(ref, ref, zsend.at[2 + which], zrecv.at[k], (ep_down, p))

    def gu_step(k, carry):
        pass_on(wgu.at[k % 2, k // 32, (k % 32) // 2], k, 0)
        return carry

    def run_gu(a, b):
        lax.fori_loop(a, b, gu_step, 0)

    place(0)
    run_gu(0, 4)
    place(1)
    run_gu(4, 7)
    place(3)
    run_gu(7, 12)
    place(2)
    run_gu(12, 18)
    shared(0)
    run_gu(18, 22)
    shared(1)
    run_gu(22, 26)
    shared(3)
    run_gu(26, 32)
    shared(2)
    run_gu(32, 52)
    hidden(0, 0)
    run_gu(52, 56)
    hidden(0, 1)
    run_gu(56, 60)
    hidden(0, 2)
    run_gu(60, 64)
    hidden(0, 3)

    me = 2 * ((p + 8 * c) % NZ) + c
    me_src = (y * 2 + c) * NX + x
    for n in range(ND):
        cols = pl.ds(n * COLS, COLS)

        def d_step(s, carry):
            pass_on(wd.at[:, s, :, cols], 64 + n * 16 + s, 1)
            return carry

        if n == 0:
            for b in range(4):
                lax.fori_loop(4 * b, 4 * b + 4, d_step, 0)
                hidden(1, b)
        else:
            lax.fori_loop(0, 16, d_step, 0)
        for b in range(4):
            at = pl.ds(b * TOK, TOK)
            v = jnp.dot(hid[0, at, :], wd[0, :, :, cols].reshape(256, COLS), preferred_element_type=F32)
            v = v + jnp.dot(hid[1, at, :], wd[1, :, :, cols].reshape(256, COLS), preferred_element_type=F32)
            res[8 * b:8 * b + 8, :, cols] = v.astype(BF).reshape(8, CAP, COLS)

        ret[me, :, cols] = res[me_src, :, cols]

        def give_back(i, carry):
            q = (me_src + i) % NE
            qy, qc, qx = q // 8, (q // 4) % 2, q % 4
            send(res.at[q, :, cols], ret.at[me, :, cols], sends.at[5], retr.at[n], (z * 2 + qc, qy * NX + qx))
            return carry

        lax.fori_loop(1, NE, give_back, 0)

    for i in (1, 3, 2):
        s = (x + i) % NX
        arrived(pin.at[s], pinr.at[s])
        for j in range(ND):
            cols = pl.ds(j * COLS, COLS)
            own[:, cols] = own[:, cols] + pin[s, :, cols].astype(F32)

    for n in range(ND):
        cols = pl.ds(n * COLS, COLS)
        arrived(ret.at[pl.ds(0, NE - 1), :, cols], retr.at[n])
        blk = ret[:, :, cols].reshape(NE * CAP, COLS)
        v = jnp.dot(wt[0], blk, preferred_element_type=F32) + jnp.dot(wt[1], blk, preferred_element_type=F32)
        outb[:, cols] = (v + own[:, cols]).astype(BF)
        pltpu.make_async_copy(outb.at[:, cols], out.at[:, cols], osem.at[n]).start()

    @pl.when(jnp.logical_not(here))
    def _():
        arrived(wgu.at[0, 0, pl.ds(0, 6)], gsend)

    @pl.when(go_up)
    def _():
        arrived(wgu, zsend.at[0])
        arrived(wd, zsend.at[1])

    @pl.when(go_down)
    def _():
        arrived(wgu, zsend.at[2])
        arrived(wd, zsend.at[3])

    arrived(meta.at[pl.ds(0, 3)], sends.at[0])
    arrived(xt.at[pl.ds(0, 3)], sends.at[1])
    arrived(sw.at[:, pl.ds(0, 3)], sends.at[2])
    arrived(rows.at[pl.ds(0, 28)], sends.at[3])
    arrived(pin.at[pl.ds(0, 3)], sends.at[4])
    arrived(ret.at[pl.ds(0, NE - 1)], sends.at[5])
    for n in range(ND):
        cols = pl.ds(n * COLS, COLS)
        pltpu.make_async_copy(outb.at[:, cols], out.at[:, cols], osem.at[n]).wait()


def body(tokens, norm_gain, expert_ids, gate_weights, expert_gate, expert_up, expert_down, shared_gate, shared_up, shared_down):
    anywhere = pl.BlockSpec(memory_space=pl.ANY)
    vmem = pl.BlockSpec(memory_space=pltpu.VMEM)
    dma = pltpu.SemaphoreType.DMA
    return pl.pallas_call(
        kernel,
        out_shape=jax.ShapeDtypeStruct((TOK, D), BF),
        in_specs=[anywhere, vmem, vmem, vmem] + [anywhere] * 6,
        out_specs=anywhere,
        scratch_shapes=[
            pltpu.VMEM((TOK, D), BF),
            pltpu.VMEM((NX, TOK, D), BF),
            pltpu.VMEM((NX, 8, TOK), F32),
            pltpu.VMEM((3, NX, 32, D), BF),
            pltpu.VMEM((NX, TOK, D), BF),
            pltpu.VMEM((NX, TOK, D), BF),
            pltpu.VMEM((TOK, D), F32),
            pltpu.VMEM((NX, 8, CAP, D), BF),
            pltpu.VMEM((NE, CAP, D), BF),
            pltpu.VMEM((2, NE * CAP, 256), BF),
            pltpu.VMEM((2, 2, 16, 16, D), BF),
            pltpu.VMEM((2, 16, 16, D), BF),
            pltpu.VMEM((NE, CAP, D), BF),
            pltpu.VMEM((NE, CAP, D), BF),
            pltpu.VMEM((2, TOK, NE * CAP), BF),
            pltpu.VMEM((TOK, D), BF),
            dma((128,)),
            dma((4,)),
            dma,
            dma,
            dma((NX,)),
            dma((NX,)),
            dma((NX,)),
            dma,
            dma((NX,)),
            dma((ND,)),
            dma((6,)),
            dma((ND,)),
        ],
        compiler_params=pltpu.CompilerParams(
            collective_id=0, has_side_effects=True, vmem_limit_bytes=48 * 1024 * 1024
        ),
    )(
        tokens,
        norm_gain.reshape(1, D),
        expert_ids.T,
        gate_weights.T,
        expert_gate.reshape(2, 16, D),
        expert_up.reshape(2, 16, D),
        expert_down.reshape(2, 16, D),
        shared_gate,
        shared_up,
        shared_down,
    )


def solution(mesh):
    in_specs = (
        P(("ep", "tp"), None),
        P(),
        P(("ep", "tp"), None),
        P(("ep", "tp"), None),
        P("ep", "tp", None),
        P("ep", "tp", None),
        P("ep", "tp", None),
        P("tp", None),
        P("tp", None),
        P("tp", None),
    )
    out_specs = P(("ep", "tp"), None)
    return jax.shard_map(body, mesh=mesh, in_specs=in_specs, out_specs=out_specs, check_vma=False)
```

```python
import functools

import jax
import jax.numpy as jnp
from jax import lax
from jax.experimental import pallas as pl
from jax.experimental.pallas import tpu as pltpu
from jax.sharding import PartitionSpec as P

EPS = 1e-06
MESH = pl.DeviceIdType.MESH
BF = jnp.bfloat16
F32 = jnp.float32
NX = 4
NZ = 16
TOK = 128
D = 2048
CAP = 16
NE = 32
COLS = 512
ND = D // COLS
NT = (((1,), (1,)), ((), ()))
STEPS = (0, 1, 2, 1)
ORDER = sorted(range(NX * NX), key=lambda i: (i // NX > 0, STEPS[i % NX] + STEPS[i // NX]))


def kernel(
    tokens, gain_in, ids_in, gw_in, eg, eu, ed, shg, shu, shd, out,
    tok, gain, ids, gw, xt, meta, sw, shid, part, pin, own, placed, rows, act, hid, wgu, wd, res, ret, wt,
    zrecv, zsend, gsend, loc, xrecv, mrecv, srecv, crecv, prow, pinr, retr, sends, credit,
):
    ep, p = lax.axis_index("ep"), lax.axis_index("tp")
    z, c = ep // 2, ep % 2
    x, y = p % NX, p // NX
    delta = (z - (p + 8 * c) + 2 * NZ) % NZ
    far = jnp.minimum(delta, NZ - delta)
    go_up = delta <= 7
    go_down = (delta == 0) | (delta >= 10)
    ep_up = ((z + 1) % NZ) * 2 + c
    ep_down = ((z + NZ - 1) % NZ) * 2 + c
    target = (z + 8 * c) % NZ
    here = p == target
    relative = ((y - target // NX + NX) % NX) * NX + (x - target % NX + NX) % NX
    rank = jnp.int32(0)
    for i, where in enumerate(ORDER):
        rank = jnp.where(relative == where, i, rank)

    def arrived(ref, sem):
        pltpu.make_async_copy(ref, ref, sem).wait()

    def send(src, dst, ssem, rsem, device):
        pltpu.make_async_remote_copy(
            src_ref=src, dst_ref=dst, send_sem=ssem, recv_sem=rsem,
            device_id=device, device_id_type=MESH,
        ).start()

    pltpu.make_async_copy(tokens, tok, loc.at[0]).start()
    pltpu.make_async_copy(ids_in, ids, loc.at[1]).start()
    pltpu.make_async_copy(gain_in, gain, loc.at[2]).start()
    pltpu.make_async_copy(gw_in, gw, loc.at[3]).start()

    barrier = pltpu.get_barrier_semaphore()

    def greet(i, carry):
        @pl.when(jnp.logical_or(i // 2 != p, i % 2 != c))
        def _():
            pl.semaphore_signal(barrier, inc=1, device_id=(z * 2 + i % 2, i // 2), device_id_type=MESH)
        return carry

    with jax.named_scope("greet"):
        lax.fori_loop(0, NE, greet, 0)
        pl.semaphore_signal(barrier, inc=1, device_id=(ep_up, p), device_id_type=MESH)
        pl.semaphore_signal(barrier, inc=1, device_id=(ep_down, p), device_id_type=MESH)

    early, late = [], []
    for m, ref in enumerate((eg, eu)):
        for h in range(2):
            early.append((ref.at[h], wgu.at[m, rank, h], rank * 4 + m * 2 + h))
    for n in range(ND):
        cols = pl.ds(n * COLS, COLS)
        late.append((ed.at[:, cols], wd.at[rank, :, cols], 64 + n * 16 + rank))

    @pl.when(here)
    def _():
        for src, dst, k in early + late:
            pltpu.make_async_copy(src, dst, zrecv.at[k]).start()

    for m, ref in enumerate((shg, shu, shd)):
        pltpu.make_async_copy(ref, sw.at[m, y], srecv.at[y]).start()

    pltpu.make_async_copy(ids_in, ids, loc.at[1]).wait()
    ids0, ids1 = ids[0:1, :], ids[1:2, :]
    e_iota = lax.broadcasted_iota(jnp.int32, (NE, TOK), 0)
    h0 = e_iota == ids0
    h1 = e_iota == ids1
    one, zero = jnp.float32(1), jnp.float32(0)
    hits = (jnp.where(h0, one, zero) + jnp.where(h1, one, zero)).astype(BF)
    earlier = jnp.where(
        lax.broadcasted_iota(jnp.int32, (TOK, TOK), 0) < lax.broadcasted_iota(jnp.int32, (TOK, TOK), 1), one, zero
    ).astype(BF)
    before = jnp.dot(hits, earlier, preferred_element_type=F32)
    slot0 = jnp.sum(jnp.where(h0, before, zero), axis=0, keepdims=True)
    slot1 = jnp.sum(jnp.where(h1, before, zero), axis=0, keepdims=True)
    pos0 = ids0.astype(F32) * CAP + slot0
    pos1 = ids1.astype(F32) * CAP + slot1
    sub = lax.broadcasted_iota(jnp.int32, (8, TOK), 0)
    meta[x] = jnp.where(sub == 0, jnp.broadcast_to(pos0, (8, TOK)), jnp.broadcast_to(pos1, (8, TOK)))

    pltpu.make_async_copy(gain_in, gain, loc.at[2]).wait()
    pltpu.make_async_copy(tokens, tok, loc.at[0]).wait()
    g = gain[...]

    def norm(i, carry):
        at = pl.ds(pl.multiple_of(i * 16, 16), 16)
        t = tok[at, :].astype(F32)
        scale = lax.rsqrt(jnp.mean(t * t, axis=-1, keepdims=True) + EPS)
        xt[x, at, :] = (t * scale * g).astype(BF)
        return carry

    with jax.named_scope("norm"):
        lax.fori_loop(0, TOK // 16, norm, 0)

    with jax.named_scope("meet"):
        pl.semaphore_wait(barrier, NE + 1)

    def gather(pieces, sem):
        @pl.when(jnp.logical_not(here))
        def _():
            for src, dst, k in pieces:
                send(src, dst, sem, zrecv.at[k], (ep, target))

    def turn(first, last):
        if first > 1:
            @pl.when(here)
            def _():
                for i in range(first, last + 1):
                    dx, dy = ORDER[i] % NX, ORDER[i] // NX
                    pl.semaphore_signal(
                        credit, inc=1, device_id=(ep, (y + dy) % NX * NX + (x + dx) % NX), device_id_type=MESH
                    )

        @pl.when(jnp.logical_and(rank >= first, rank <= last))
        def _():
            if first > 1:
                with jax.named_scope("credit"):
                    pl.semaphore_wait(credit, 1)
            for src, dst, k in early:
                send(src, dst, gsend.at[0], zrecv.at[k], (ep, target))

    turn(1, 4)

    def share_tokens():
        for i in (1, 3, 2):
            peer = (ep, y * NX + (x + i) % NX)
            send(meta.at[x], meta.at[x], sends.at[0], mrecv.at[x], peer)
            send(xt.at[x], xt.at[x], sends.at[1], xrecv.at[x], peer)

    def pass_on(ref, k, which):
        arrived(ref, zrecv.at[k])

        @pl.when(go_up)
        def _():
            send(ref, ref, zsend.at[which], zrecv.at[k], (ep_up, p))

        @pl.when(go_down)
        def _():
            send(ref, ref, zsend.at[2 + which], zrecv.at[k], (ep_down, p))

    def gu_step(i, carry):
        pass_on(wgu.at[(i // 2) % 2, i // 4, i % 2], i, 0)
        return carry

    def d_step(i, carry):
        n, s = (i - 64) // 16, i % 16
        pass_on(wd.at[s, :, pl.ds(pl.multiple_of(n * COLS, COLS), COLS)], i, 1)
        return carry

    done = [0]

    def stream(time=None, least=0, more=0):
        a = done[0]
        b = jnp.minimum(a + jnp.where(go_up | go_down, more, 0), 128)
        b = jnp.maximum(b, least)
        if time is not None:
            left = time - 10 - (34 - 6 * c) * far
            k = jnp.where(left < 451, jnp.maximum(left, 0) * 10 // 71, 64 + (left - 451) * 10 // 36)
            b = jnp.maximum(b, jnp.minimum(k, 128))
        with jax.named_scope("s"):
            lax.fori_loop(jnp.minimum(a, 64), jnp.minimum(b, 64), gu_step, 0)
            lax.fori_loop(jnp.maximum(a, 64), jnp.maximum(b, 64), d_step, 0)
        done[0] = b

    def weigh():
        pltpu.make_async_copy(gw_in, gw, loc.at[3]).wait()
        slot_iota = lax.broadcasted_iota(jnp.int32, (NE * CAP, TOK), 0).astype(F32)
        w = jnp.where(slot_iota == pos0, gw[0:1, :], zero) + jnp.where(slot_iota == pos1, gw[1:2, :], zero)
        w = w.T
        w_hi = w.astype(BF)
        wt[0] = w_hi
        wt[1] = (w - w_hi.astype(F32)).astype(BF)

    def place(i):
        with jax.named_scope(f"place{i}"):
            s = (x + i) % NX
            if i:
                arrived(meta.at[s], mrecv.at[s])
                arrived(xt.at[s], xrecv.at[s])
            row = lax.broadcasted_iota(jnp.int32, (TOK, TOK), 0)
            dest, slot = row >> 4, row & 15
            dy, dc = dest >> 1, dest & 1
            expert = 2 * ((4 * dy + x + 8 * dc) & 15) + dc
            aim = (expert * CAP + slot).astype(F32)
            m = meta[s]
            onehot = jnp.where((aim == m[0:1, :]) | (aim == m[1:2, :]), one, zero).astype(BF)
            for j in range(ND):
                cols = pl.ds(j * COLS, COLS)
                placed[s, :, :, cols] = (
                    jnp.dot(onehot, xt[s, :, cols], preferred_element_type=F32).astype(BF).reshape(8, CAP, COLS)
                )
            src = (y * 2 + c) * NX + s
            rows[src] = placed[s, y * 2 + c]
            for q in range(1, 8):
                dest = (y * 2 + c + q) % 8
                send(placed.at[s, dest], rows.at[src], sends.at[3], prow, (z * 2 + dest % 2, (dest // 2) * NX + x))

    def share_weights():
        for i in (1, 3, 2):
            peer = (ep, ((y + i) % NX) * NX + x)
            for m, ref in enumerate((shg, shu, shd)):
                send(ref.at[c], sw.at[m, y, c], sends.at[2], srecv.at[y], peer)

    def cross():
        with jax.named_scope("cross"):
            for i in (1, 3, 2):
                s = (y + i) % NX
                arrived(sw.at[:, s, c], srecv.at[s])
                send(sw.at[:, s, c], sw.at[:, s, c], sends.at[6], crecv.at[s], (z * 2 + 1 - c, p))

    def shared_up(i):
        with jax.named_scope("sharedu"):
            s = (x + i) % NX
            if i == 0:
                arrived(sw.at[:, y], srecv.at[y])
                for q in range(1, NX):
                    arrived(sw.at[:, (y + q) % NX, 1 - c], crecv.at[(y + q) % NX])
            blk = xt[s]
            a = lax.dot_general(blk, sw[0].reshape(TOK, D), NT, preferred_element_type=F32)
            b = lax.dot_general(blk, sw[1].reshape(TOK, D), NT, preferred_element_type=F32)
            shid[...] = (a / (1.0 + jnp.exp(-a)) * b).astype(BF)

    def shared_down(i):
        with jax.named_scope("sharedd"):
            s = (x + i) % NX
            down = sw.at[2]
            for j in range(ND):
                cols = pl.ds(j * COLS, COLS)
                v = jnp.dot(shid[...], down[:, :, :, cols].reshape(TOK, COLS), preferred_element_type=F32)
                if i == 0:
                    own[:, cols] = v
                else:
                    part[s, :, cols] = v.astype(BF)
            if i:
                send(part.at[s], pin.at[x], sends.at[4], pinr.at[x], (ep, y * NX + s))

    HALF = NE * CAP // 2

    def hidden(r, b, m):
        with jax.named_scope("hidden"):
            blk = rows[16 * b:16 * b + 16].reshape(HALF, D)
            v = lax.dot_general(blk, wgu[m, 8 * r:8 * r + 8].reshape(256, D), NT, preferred_element_type=F32)
            if m == 0:
                act[...] = v / (1.0 + jnp.exp(-v))
            else:
                hid[r, b * HALF:(b + 1) * HALF, :] = (act[...] * v).astype(BF)

    me = 2 * ((p + 8 * c) % NZ) + c
    me_src = (y * 2 + c) * NX + x

    def result(n):
        with jax.named_scope("result"):
            cols = pl.ds(n * COLS, COLS)
            for b in range(2):
                at = pl.ds(b * HALF, HALF)
                v = jnp.dot(hid[0, at, :], wd[0:8, :, cols].reshape(256, COLS), preferred_element_type=F32)
                v = v + jnp.dot(hid[1, at, :], wd[8:16, :, cols].reshape(256, COLS), preferred_element_type=F32)
                res[16 * b:16 * b + 16, :, cols] = v.astype(BF).reshape(16, CAP, COLS)
            ret[me, :, cols] = res[me_src, :, cols]

    def give_back(n, a, b):
        cols = pl.ds(n * COLS, COLS)

        def one_block(i, carry):
            q = (me_src + i) % NE
            qy, qc, qx = q // 8, (q // 4) % 2, q % 4
            send(res.at[q, :, cols], ret.at[me, :, cols], sends.at[5], retr.at[n], (z * 2 + qc, qy * NX + qx))
            return carry

        with jax.named_scope("give"):
            lax.fori_loop(a, b, one_block, 0)

    def take_part(i):
        s = (x + i) % NX
        with jax.named_scope("pin"):
            arrived(pin.at[s], pinr.at[s])
            for j in range(ND):
                cols = pl.ds(j * COLS, COLS)
                own[:, cols] = own[:, cols] + pin[s, :, cols].astype(F32)

    weigh()
    stream(time=50)
    turn(5, 8)
    stream(time=110)
    turn(9, 12)
    stream(time=130)

    @pl.when(far > 3)
    def _():
        pl.delay(11000)

    share_tokens()
    place(0)
    stream(time=170)
    turn(13, 15)
    share_weights()
    stream(time=280)
    gather(late, gsend.at[1])
    stream(time=455)
    place(1)
    stream(time=460)
    place(3)
    stream(time=475)
    place(2)
    stream(time=510)
    cross()
    stream(time=560)
    for i in (0, 1, 3, 2):
        shared_up(i)
        stream(more=2)
        shared_down(i)
        stream(more=2)
    stream(time=690, least=32)
    with jax.named_scope("wait_rows"):
        arrived(rows.at[pl.ds(0, 28)], prow)
    stream(least=64)
    for r in range(2):
        for b in range(2):
            for m in range(2):
                hidden(r, b, m)
                stream(more=3)
    for n in range(ND):
        stream(least=64 + 16 * n + 16)
        result(n)
        stream(more=3)
        give_back(n, 1, 16)
        stream(more=3)
        give_back(n, 16, NE)
        stream(more=3)
    for i in (1, 3, 2):
        take_part(i)

    for n in range(ND):
        cols = pl.ds(n * COLS, COLS)
        with jax.named_scope(f"wait_ret{n}"):
            arrived(ret.at[pl.ds(0, NE - 1), :, cols], retr.at[n])
        with jax.named_scope("combine"):
            blk = ret[:, :, cols].reshape(NE * CAP, COLS)
            v = jnp.dot(wt[0], blk, preferred_element_type=F32) + jnp.dot(wt[1], blk, preferred_element_type=F32)
            out[:, cols] = (v + own[:, cols]).astype(BF)

    @pl.when(jnp.logical_not(here))
    def _():
        arrived(wgu.at[0, pl.ds(0, 2)], gsend.at[0])
        arrived(wd.at[0], gsend.at[1])

    @pl.when(go_up)
    def _():
        arrived(wgu, zsend.at[0])
        arrived(wd, zsend.at[1])

    @pl.when(go_down)
    def _():
        arrived(wgu, zsend.at[2])
        arrived(wd, zsend.at[3])

    arrived(meta.at[pl.ds(0, 3)], sends.at[0])
    arrived(xt.at[pl.ds(0, 3)], sends.at[1])
    arrived(sw.at[:, pl.ds(0, 3), 0], sends.at[2])
    arrived(sw.at[:, pl.ds(0, 3), 0], sends.at[6])
    arrived(rows.at[pl.ds(0, 28)], sends.at[3])
    arrived(pin.at[pl.ds(0, 3)], sends.at[4])
    arrived(ret.at[pl.ds(0, NE - 1)], sends.at[5])


def body(tokens, norm_gain, expert_ids, gate_weights, expert_gate, expert_up, expert_down, shared_gate, shared_up, shared_down):
    anywhere = pl.BlockSpec(memory_space=pl.ANY)
    dma = pltpu.SemaphoreType.DMA
    return pl.pallas_call(
        kernel,
        out_shape=jax.ShapeDtypeStruct((TOK, D), BF),
        in_specs=[anywhere] * 10,
        out_specs=pl.BlockSpec(memory_space=pltpu.VMEM),
        scratch_shapes=[
            pltpu.VMEM((TOK, D), BF),
            pltpu.VMEM((1, D), F32),
            pltpu.VMEM((2, TOK), jnp.int32),
            pltpu.VMEM((2, TOK), F32),
            pltpu.VMEM((NX, TOK, D), BF),
            pltpu.VMEM((NX, 8, TOK), F32),
            pltpu.VMEM((3, NX, 2, 16, D), BF),
            pltpu.VMEM((TOK, TOK), BF),
            pltpu.VMEM((NX, TOK, D), BF),
            pltpu.VMEM((NX, TOK, D), BF),
            pltpu.VMEM((TOK, D), F32),
            pltpu.VMEM((NX, 8, CAP, D), BF),
            pltpu.VMEM((NE, CAP, D), BF),
            pltpu.VMEM((NE * CAP // 2, 256), F32),
            pltpu.VMEM((2, NE * CAP, 256), BF),
            pltpu.VMEM((2, 16, 2, 16, D), BF),
            pltpu.VMEM((16, 32, D), BF),
            pltpu.VMEM((NE, CAP, D), BF),
            pltpu.VMEM((NE, CAP, D), BF),
            pltpu.VMEM((2, TOK, NE * CAP), BF),
            dma((128,)),
            dma((4,)),
            dma((2,)),
            dma((4,)),
            dma((NX,)),
            dma((NX,)),
            dma((NX,)),
            dma((NX,)),
            dma,
            dma((NX,)),
            dma((ND,)),
            dma((7,)),
            pltpu.SemaphoreType.REGULAR,
        ],
        compiler_params=pltpu.CompilerParams(
            collective_id=0, has_side_effects=True, vmem_limit_bytes=48000 * 1024
        ),
    )(
        *[pltpu.with_memory_space_constraint(a, pltpu.HBM) for a in (
            tokens,
        norm_gain.reshape(1, D),
        expert_ids.T,
        gate_weights.T,
        expert_gate.reshape(2, 16, D),
        expert_up.reshape(2, 16, D),
        expert_down.reshape(32, D),
        shared_gate.reshape(2, 16, D),
        shared_up.reshape(2, 16, D),
        shared_down.reshape(2, 16, D),
        )]
    )


def solution(mesh):
    in_specs = (
        P(("ep", "tp"), None),
        P(),
        P(("ep", "tp"), None),
        P(("ep", "tp"), None),
        P("ep", "tp", None),
        P("ep", "tp", None),
        P("ep", "tp", None),
        P("tp", None),
        P("tp", None),
        P("tp", None),
    )
    out_specs = P(("ep", "tp"), None)
    return jax.shard_map(body, mesh=mesh, in_specs=in_specs, out_specs=out_specs, check_vma=False)
```

```python
import functools

import jax
import jax.numpy as jnp
from jax import lax
from jax.experimental import pallas as pl
from jax.experimental.pallas import tpu as pltpu
from jax.sharding import PartitionSpec as P

EPS = 1e-06
MESH = pl.DeviceIdType.MESH
BF = jnp.bfloat16
F32 = jnp.float32
NX = 4
NZ = 16
TOK = 128
D = 2048
CAP = 16
NE = 32
COLS = 512
ND = D // COLS
NT = (((1,), (1,)), ((), ()))
STEPS = (0, 1, 2, 1)
ORDER = sorted(range(NX * NX), key=lambda i: (i // NX > 0, STEPS[i % NX] + STEPS[i // NX]))


def kernel(
    tokens, gain_in, ids_in, gw_in, eg, eu, ed, shg, shu, shd, out,
    tok, gain, ids, gw, xt, meta, sw, shid, part, pin, own, placed, rows, act, hid, wgu, wd, res, ret, wt,
    zrecv, zsend, gsend, loc, xrecv, mrecv, srecv, crecv, prow, pinr, retr, sends, credit,
):
    ep, p = lax.axis_index("ep"), lax.axis_index("tp")
    z, c = ep // 2, ep % 2
    x, y = p % NX, p // NX
    delta = (z - (p + 8 * c) + 2 * NZ) % NZ
    far = jnp.minimum(delta, NZ - delta)
    go_up = delta <= 7
    go_down = (delta == 0) | (delta >= 10)
    ep_up = ((z + 1) % NZ) * 2 + c
    ep_down = ((z + NZ - 1) % NZ) * 2 + c
    target = (z + 8 * c) % NZ
    here = p == target
    relative = ((y - target // NX + NX) % NX) * NX + (x - target % NX + NX) % NX
    rank = jnp.int32(0)
    for i, where in enumerate(ORDER):
        rank = jnp.where(relative == where, i, rank)

    def arrived(ref, sem):
        pltpu.make_async_copy(ref, ref, sem).wait()

    def send(src, dst, ssem, rsem, device):
        pltpu.make_async_remote_copy(
            src_ref=src, dst_ref=dst, send_sem=ssem, recv_sem=rsem,
            device_id=device, device_id_type=MESH,
        ).start()

    pltpu.make_async_copy(tokens, tok, loc.at[0]).start()
    pltpu.make_async_copy(ids_in, ids, loc.at[1]).start()
    pltpu.make_async_copy(gain_in, gain, loc.at[2]).start()
    pltpu.make_async_copy(gw_in, gw, loc.at[3]).start()

    barrier = pltpu.get_barrier_semaphore()

    def greet(i, carry):
        @pl.when(jnp.logical_or(i // 2 != p, i % 2 != c))
        def _():
            pl.semaphore_signal(barrier, inc=1, device_id=(z * 2 + i % 2, i // 2), device_id_type=MESH)
        return carry

    with jax.named_scope("greet"):
        lax.fori_loop(0, NE, greet, 0)
        pl.semaphore_signal(barrier, inc=1, device_id=(ep_up, p), device_id_type=MESH)
        pl.semaphore_signal(barrier, inc=1, device_id=(ep_down, p), device_id_type=MESH)

    early, late = [], []
    for m, ref in enumerate((eg, eu)):
        for h in range(2):
            early.append((ref.at[h], wgu.at[m, rank, h], rank * 4 + m * 2 + h))
    for n in range(ND):
        cols = pl.ds(n * COLS, COLS)
        late.append((ed.at[:, cols], wd.at[rank, :, cols], 64 + n * 16 + rank))

    @pl.when(here)
    def _():
        for src, dst, k in early + late:
            pltpu.make_async_copy(src, dst, zrecv.at[k]).start()

    for m, ref in enumerate((shg, shu, shd)):
        pltpu.make_async_copy(ref, sw.at[m, y], srecv.at[y]).start()

    pltpu.make_async_copy(ids_in, ids, loc.at[1]).wait()
    ids0, ids1 = ids[0:1, :], ids[1:2, :]
    e_iota = lax.broadcasted_iota(jnp.int32, (NE, TOK), 0)
    h0 = e_iota == ids0
    h1 = e_iota == ids1
    one, zero = jnp.float32(1), jnp.float32(0)
    hits = (jnp.where(h0, one, zero) + jnp.where(h1, one, zero)).astype(BF)
    earlier = jnp.where(
        lax.broadcasted_iota(jnp.int32, (TOK, TOK), 0) < lax.broadcasted_iota(jnp.int32, (TOK, TOK), 1), one, zero
    ).astype(BF)
    before = jnp.dot(hits, earlier, preferred_element_type=F32)
    slot0 = jnp.sum(jnp.where(h0, before, zero), axis=0, keepdims=True)
    slot1 = jnp.sum(jnp.where(h1, before, zero), axis=0, keepdims=True)
    pos0 = ids0.astype(F32) * CAP + slot0
    pos1 = ids1.astype(F32) * CAP + slot1
    sub = lax.broadcasted_iota(jnp.int32, (8, TOK), 0)
    meta[x] = jnp.where(sub == 0, jnp.broadcast_to(pos0, (8, TOK)), jnp.broadcast_to(pos1, (8, TOK)))

    pltpu.make_async_copy(gain_in, gain, loc.at[2]).wait()
    pltpu.make_async_copy(tokens, tok, loc.at[0]).wait()
    g = gain[...]

    def norm(i, carry):
        at = pl.ds(pl.multiple_of(i * 16, 16), 16)
        t = tok[at, :].astype(F32)
        scale = lax.rsqrt(jnp.mean(t * t, axis=-1, keepdims=True) + EPS)
        xt[x, at, :] = (t * scale * g).astype(BF)
        return carry

    with jax.named_scope("norm"):
        lax.fori_loop(0, TOK // 16, norm, 0)

    with jax.named_scope("meet"):
        pl.semaphore_wait(barrier, NE + 1)

    def gather(pieces, sem):
        @pl.when(jnp.logical_not(here))
        def _():
            for src, dst, k in pieces:
                send(src, dst, sem, zrecv.at[k], (ep, target))

    def turn(first, last):
        if first > 1:
            @pl.when(here)
            def _():
                for i in range(first, last + 1):
                    dx, dy = ORDER[i] % NX, ORDER[i] // NX
                    pl.semaphore_signal(
                        credit, inc=1, device_id=(ep, (y + dy) % NX * NX + (x + dx) % NX), device_id_type=MESH
                    )

        @pl.when(jnp.logical_and(rank >= first, rank <= last))
        def _():
            if first > 1:
                with jax.named_scope("credit"):
                    pl.semaphore_wait(credit, 1)
            for src, dst, k in early:
                send(src, dst, gsend.at[0], zrecv.at[k], (ep, target))

    turn(1, 4)

    def share_tokens():
        for i in (1, 3, 2):
            peer = (ep, y * NX + (x + i) % NX)
            send(meta.at[x], meta.at[x], sends.at[0], mrecv.at[x], peer)
            send(xt.at[x], xt.at[x], sends.at[1], xrecv.at[x], peer)

    def pass_on(ref, k, which):
        arrived(ref, zrecv.at[k])

        @pl.when(go_up)
        def _():
            send(ref, ref, zsend.at[which], zrecv.at[k], (ep_up, p))

        @pl.when(go_down)
        def _():
            send(ref, ref, zsend.at[2 + which], zrecv.at[k], (ep_down, p))

    def gu_step(i, carry):
        pass_on(wgu.at[(i // 2) % 2, i // 4, i % 2], i, 0)
        return carry

    def d_step(i, carry):
        n, s = (i - 64) // 16, i % 16
        pass_on(wd.at[s, :, pl.ds(pl.multiple_of(n * COLS, COLS), COLS)], i, 1)
        return carry

    done = [0]

    def stream(time=None, least=0, more=0):
        a = done[0]
        b = jnp.minimum(a + jnp.where(go_up | go_down, more, 0), 128)
        b = jnp.maximum(b, least)
        if time is not None:
            left = time - 10 - (34 - 6 * c) * far
            k = jnp.where(left < 451, jnp.maximum(left, 0) * 10 // 71, 64 + (left - 451) * 10 // 36)
            b = jnp.maximum(b, jnp.minimum(k, 128))
        with jax.named_scope("s"):
            lax.fori_loop(jnp.minimum(a, 64), jnp.minimum(b, 64), gu_step, 0)
            lax.fori_loop(jnp.maximum(a, 64), jnp.maximum(b, 64), d_step, 0)
        done[0] = b

    def weigh():
        pltpu.make_async_copy(gw_in, gw, loc.at[3]).wait()
        slot_iota = lax.broadcasted_iota(jnp.int32, (NE * CAP, TOK), 0).astype(F32)
        w = jnp.where(slot_iota == pos0, gw[0:1, :], zero) + jnp.where(slot_iota == pos1, gw[1:2, :], zero)
        w = w.T
        w_hi = w.astype(BF)
        wt[0] = w_hi
        wt[1] = (w - w_hi.astype(F32)).astype(BF)

    def place(i):
        with jax.named_scope(f"place{i}"):
            s = (x + i) % NX
            if i:
                arrived(meta.at[s], mrecv.at[s])
                arrived(xt.at[s], xrecv.at[s])
            row = lax.broadcasted_iota(jnp.int32, (TOK, TOK), 0)
            dest, slot = row >> 4, row & 15
            dy, dc = dest >> 1, dest & 1
            expert = 2 * ((4 * dy + x + 8 * dc) & 15) + dc
            aim = (expert * CAP + slot).astype(F32)
            m = meta[s]
            onehot = jnp.where((aim == m[0:1, :]) | (aim == m[1:2, :]), one, zero).astype(BF)
            for j in range(ND):
                cols = pl.ds(j * COLS, COLS)
                placed[s, :, :, cols] = (
                    jnp.dot(onehot, xt[s, :, cols], preferred_element_type=F32).astype(BF).reshape(8, CAP, COLS)
                )
            src = (y * 2 + c) * NX + s
            rows[src] = placed[s, y * 2 + c]
            for q in range(1, 8):
                dest = (y * 2 + c + q) % 8
                send(placed.at[s, dest], rows.at[src], sends.at[3], prow, (z * 2 + dest % 2, (dest // 2) * NX + x))

    def share_weights():
        for i in (1, 3, 2):
            peer = (ep, ((y + i) % NX) * NX + x)
            for m, ref in enumerate((shg, shu, shd)):
                send(ref.at[c], sw.at[m, y, c], sends.at[2], srecv.at[y], peer)

    def cross():
        with jax.named_scope("cross"):
            for i in (1, 3, 2):
                s = (y + i) % NX
                arrived(sw.at[:, s, c], srecv.at[s])
                send(sw.at[:, s, c], sw.at[:, s, c], sends.at[6], crecv.at[s], (z * 2 + 1 - c, p))

    def shared_up(i):
        with jax.named_scope("sharedu"):
            s = (x + i) % NX
            if i == 0:
                arrived(sw.at[:, y], srecv.at[y])
                for q in range(1, NX):
                    arrived(sw.at[:, (y + q) % NX, 1 - c], crecv.at[(y + q) % NX])
            blk = xt[s]
            a = lax.dot_general(blk, sw[0].reshape(TOK, D), NT, preferred_element_type=F32)
            b = lax.dot_general(blk, sw[1].reshape(TOK, D), NT, preferred_element_type=F32)
            shid[...] = (a / (1.0 + jnp.exp(-a)) * b).astype(BF)

    def shared_down(i):
        with jax.named_scope("sharedd"):
            s = (x + i) % NX
            down = sw.at[2]
            for j in range(ND):
                cols = pl.ds(j * COLS, COLS)
                v = jnp.dot(shid[...], down[:, :, :, cols].reshape(TOK, COLS), preferred_element_type=F32)
                if i == 0:
                    own[:, cols] = v
                else:
                    part[s, :, cols] = v.astype(BF)
            if i:
                send(part.at[s], pin.at[x], sends.at[4], pinr.at[x], (ep, y * NX + s))

    HALF = NE * CAP // 2

    def hidden(r, b, m):
        with jax.named_scope("hidden"):
            blk = rows[16 * b:16 * b + 16].reshape(HALF, D)
            v = lax.dot_general(blk, wgu[m, 8 * r:8 * r + 8].reshape(256, D), NT, preferred_element_type=F32)
            if m == 0:
                act[...] = v / (1.0 + jnp.exp(-v))
            else:
                hid[r, b * HALF:(b + 1) * HALF, :] = (act[...] * v).astype(BF)

    me = 2 * ((p + 8 * c) % NZ) + c
    me_src = (y * 2 + c) * NX + x

    def result(n):
        with jax.named_scope("result"):
            cols = pl.ds(n * COLS, COLS)
            for b in range(2):
                at = pl.ds(b * HALF, HALF)
                v = jnp.dot(hid[0, at, :], wd[0:8, :, cols].reshape(256, COLS), preferred_element_type=F32)
                v = v + jnp.dot(hid[1, at, :], wd[8:16, :, cols].reshape(256, COLS), preferred_element_type=F32)
                res[16 * b:16 * b + 16, :, cols] = v.astype(BF).reshape(16, CAP, COLS)
            ret[me, :, cols] = res[me_src, :, cols]

    def give_back(n, a, b):
        cols = pl.ds(n * COLS, COLS)

        def one_block(i, carry):
            q = (me_src + i) % NE
            qy, qc, qx = q // 8, (q // 4) % 2, q % 4
            send(res.at[q, :, cols], ret.at[me, :, cols], sends.at[5], retr.at[n], (z * 2 + qc, qy * NX + qx))
            return carry

        with jax.named_scope("give"):
            lax.fori_loop(a, b, one_block, 0)

    def take_part(i):
        s = (x + i) % NX
        with jax.named_scope("pin"):
            arrived(pin.at[s], pinr.at[s])
            for j in range(ND):
                cols = pl.ds(j * COLS, COLS)
                own[:, cols] = own[:, cols] + pin[s, :, cols].astype(F32)

    weigh()
    stream(time=40)
    turn(5, 8)
    stream(time=95)
    turn(9, 12)
    stream(time=130)

    @pl.when(far > 3)
    def _():
        pl.delay(11000)

    share_tokens()
    place(0)
    stream(time=150)
    turn(13, 15)
    share_weights()
    stream(time=280)
    gather(late, gsend.at[1])
    stream(time=455)
    place(1)
    stream(time=460)
    place(3)
    stream(time=475)
    place(2)
    stream(time=510)
    cross()
    stream(time=560)
    for i in (0, 1, 3, 2):
        shared_up(i)
        stream(more=2)
        shared_down(i)
        stream(more=2)
    stream(time=690, least=32)
    with jax.named_scope("wait_rows"):
        arrived(rows.at[pl.ds(0, 28)], prow)
    stream(least=64)
    for r in range(2):
        for b in range(2):
            for m in range(2):
                hidden(r, b, m)
                stream(more=3)
    for n in range(ND):
        stream(least=64 + 16 * n + 16)
        result(n)
        stream(more=3)
        give_back(n, 1, 16)
        stream(more=3)
        give_back(n, 16, NE)
        stream(more=3)
    for i in (1, 3, 2):
        take_part(i)

    for n in range(ND):
        cols = pl.ds(n * COLS, COLS)
        with jax.named_scope(f"wait_ret{n}"):
            arrived(ret.at[pl.ds(0, NE - 1), :, cols], retr.at[n])
        with jax.named_scope("combine"):
            blk = ret[:, :, cols].reshape(NE * CAP, COLS)
            v = jnp.dot(wt[0], blk, preferred_element_type=F32) + jnp.dot(wt[1], blk, preferred_element_type=F32)
            out[:, cols] = (v + own[:, cols]).astype(BF)

    @pl.when(jnp.logical_not(here))
    def _():
        arrived(wgu.at[0, pl.ds(0, 2)], gsend.at[0])
        arrived(wd.at[0], gsend.at[1])

    @pl.when(go_up)
    def _():
        arrived(wgu, zsend.at[0])
        arrived(wd, zsend.at[1])

    @pl.when(go_down)
    def _():
        arrived(wgu, zsend.at[2])
        arrived(wd, zsend.at[3])

    arrived(meta.at[pl.ds(0, 3)], sends.at[0])
    arrived(xt.at[pl.ds(0, 3)], sends.at[1])
    arrived(sw.at[:, pl.ds(0, 3), 0], sends.at[2])
    arrived(sw.at[:, pl.ds(0, 3), 0], sends.at[6])
    arrived(rows.at[pl.ds(0, 28)], sends.at[3])
    arrived(pin.at[pl.ds(0, 3)], sends.at[4])
    arrived(ret.at[pl.ds(0, NE - 1)], sends.at[5])


def body(tokens, norm_gain, expert_ids, gate_weights, expert_gate, expert_up, expert_down, shared_gate, shared_up, shared_down):
    anywhere = pl.BlockSpec(memory_space=pl.ANY)
    dma = pltpu.SemaphoreType.DMA
    return pl.pallas_call(
        kernel,
        out_shape=jax.ShapeDtypeStruct((TOK, D), BF),
        in_specs=[anywhere] * 10,
        out_specs=pl.BlockSpec(memory_space=pltpu.VMEM),
        scratch_shapes=[
            pltpu.VMEM((TOK, D), BF),
            pltpu.VMEM((1, D), F32),
            pltpu.VMEM((2, TOK), jnp.int32),
            pltpu.VMEM((2, TOK), F32),
            pltpu.VMEM((NX, TOK, D), BF),
            pltpu.VMEM((NX, 8, TOK), F32),
            pltpu.VMEM((3, NX, 2, 16, D), BF),
            pltpu.VMEM((TOK, TOK), BF),
            pltpu.VMEM((NX, TOK, D), BF),
            pltpu.VMEM((NX, TOK, D), BF),
            pltpu.VMEM((TOK, D), F32),
            pltpu.VMEM((NX, 8, CAP, D), BF),
            pltpu.VMEM((NE, CAP, D), BF),
            pltpu.VMEM((NE * CAP // 2, 256), F32),
            pltpu.VMEM((2, NE * CAP, 256), BF),
            pltpu.VMEM((2, 16, 2, 16, D), BF),
            pltpu.VMEM((16, 32, D), BF),
            pltpu.VMEM((NE, CAP, D), BF),
            pltpu.VMEM((NE, CAP, D), BF),
            pltpu.VMEM((2, TOK, NE * CAP), BF),
            dma((128,)),
            dma((4,)),
            dma((2,)),
            dma((4,)),
            dma((NX,)),
            dma((NX,)),
            dma((NX,)),
            dma((NX,)),
            dma,
            dma((NX,)),
            dma((ND,)),
            dma((7,)),
            pltpu.SemaphoreType.REGULAR,
        ],
        compiler_params=pltpu.CompilerParams(
            collective_id=0, has_side_effects=True, vmem_limit_bytes=48000 * 1024
        ),
    )(
        *[pltpu.with_memory_space_constraint(a, pltpu.HBM) for a in (
            tokens,
        norm_gain.reshape(1, D),
        expert_ids.T,
        gate_weights.T,
        expert_gate.reshape(2, 16, D),
        expert_up.reshape(2, 16, D),
        expert_down.reshape(32, D),
        shared_gate.reshape(2, 16, D),
        shared_up.reshape(2, 16, D),
        shared_down.reshape(2, 16, D),
        )]
    )


def solution(mesh):
    in_specs = (
        P(("ep", "tp"), None),
        P(),
        P(("ep", "tp"), None),
        P(("ep", "tp"), None),
        P("ep", "tp", None),
        P("ep", "tp", None),
        P("ep", "tp", None),
        P("tp", None),
        P("tp", None),
        P("tp", None),
    )
    out_specs = P(("ep", "tp"), None)
    return jax.shard_map(body, mesh=mesh, in_specs=in_specs, out_specs=out_specs, check_vma=False)
```
